1024 devices in a mesh: gr: 2 (over z_hi), sp: 64 (over z_lo, y), tp: 8 (over x, core).
Axes of the slice: x: 4, y: 8, z: 16 (z_hi: 2, z_lo: 8; z = z_hi * 8 + z_lo), core: 2. Of those that a mesh axis runs over, the one named last changes fastest.
Arguments:
- layer_input: bfloat16 [2, 98304, 2048], P('gr', ('sp', 'tp')), may hold values from -6 to 6
- key_weight: bfloat16 [2048, 2048], P(None, 'tp'), may hold values from -0.125 to 0.125
- value_weight: bfloat16 [2048, 2048], P(None, 'tp'), may hold values from -0.125 to 0.125
- new_queries: bfloat16 [2, 2048], P('gr', 'tp'), may hold values from -280 to 280
- lambdas: float32 [16], P('tp'), may hold values from 0.3 to 0.8
- head_gain: float32 [128], replicated, may hold values from 0.1 to 1.9
- out_weight: bfloat16 [2048, 2048], P('tp'), may hold values from -0.125 to 0.125
Outputs:
- key_cache: bfloat16 [2, 98304, 2048], P('gr', 'sp', 'tp')
- value_cache: bfloat16 [2, 98304, 2048], P('gr', 'sp', 'tp')
- mixed: bfloat16 [2, 2048], P('gr', 'tp')
The draws below stay inside these ranges and needn't reach their ends.
All inputs are finite; a program needn't handle non-finite values.
Results may differ from the reference program's by a relative error of at most 0.03.
Values may be sent and summed in bfloat16 or wider, within the bound.
A program may use at most 64 MiB of HBM per device.

```python
import jax
import jax.numpy as jnp
from jax import lax

D = 2048
HEADS = 16
HEAD_DIM = 64
ROWS = 192
LEN = 98304
SEQS = 2
N_SP = 64
N_TP = 8


def draw_new_queries(key, part):
    drawn_rows = jax.random.normal(jax.random.fold_in(key, 11), (SEQS, HEADS * 2 * HEAD_DIM), jnp.float32)
    drawn_rows = jnp.clip(drawn_rows, -4.0, 4.0) * 1.7
    return drawn_rows.astype(jnp.bfloat16)


def block_scale(key, shape, pieces, low, high):
    factor_of, own = 1.0, jax.random.fold_in(key, 6)
    for position, parts in pieces:
        heights = jnp.exp(jax.random.uniform(jax.random.fold_in(own, position), (parts,), jnp.float32, low / len(pieces), high / len(pieces)))
        factor_of = factor_of * jnp.repeat(heights, shape[position] // parts).reshape([-1 if axis == position else 1 for axis in range(len(shape))])
    return factor_of


def gaussian(own_key, dims, scale, most, cuts=(), kind=jnp.bfloat16):
    loudness = block_scale(own_key, dims, cuts, -0.22, 0.18) if cuts else 1.0
    entries = jax.random.normal(own_key, dims, jnp.float32) * scale * loudness
    return jnp.minimum(jnp.maximum(entries, -most), most).astype(kind)


def setup_inputs(seed: int = 0) -> dict:
    arg_keys = jax.random.split(jax.random.key(seed), 8)
    return {
        "layer_input": gaussian(arg_keys[0], (SEQS, LEN, D), 1.0, 6.0, ((0, 2), (1, 512))),
        "key_weight": gaussian(arg_keys[1], (D, HEADS * 2 * HEAD_DIM), D ** -0.5, 0.125, ((1, 8),)),
        "value_weight": gaussian(arg_keys[2], (D, HEADS * 2 * HEAD_DIM), D ** -0.5, 0.125, ((1, 8),)),
        "new_queries": draw_new_queries(jax.random.fold_in(arg_keys[7], 71), 0),
        "lambdas": jnp.clip(0.3 + 0.5 * jax.random.uniform(arg_keys[4], (HEADS,), jnp.float32) ** block_scale(arg_keys[4], (HEADS,), ((0, 8),), -0.2, 0.2), 0.3, 0.8),
        "head_gain": jnp.clip(1.0 + 0.18 * jax.random.normal(arg_keys[5], (2 * HEAD_DIM,), jnp.float32), 0.1, 1.9),
        "out_weight": gaussian(arg_keys[6], (HEADS * 2 * HEAD_DIM, D), (HEADS * 2 * HEAD_DIM) ** -0.5, 0.125, ((0, 8),)),
    }


def rotate(raw_keys, positions, head_dim):
    inverse = 1.0 / 10000.0 ** (jnp.arange(0, head_dim, 2, dtype=jnp.float32) / head_dim)
    angles = positions.astype(jnp.float32)[:, None] * inverse[None, :]
    angles = jnp.concatenate([angles, angles], axis=-1)
    cosine = jnp.cos(angles)[:, None, :]
    sine = jnp.sin(angles)[:, None, :]
    first_half, second_half = jnp.split(raw_keys, 2, axis=-1)
    turned = jnp.concatenate([-second_half, first_half], axis=-1)
    return raw_keys * cosine + turned * sine

def reference(layer_input, key_weight, value_weight, new_queries, lambdas, head_gain, out_weight):
    block_rows = ROWS * N_TP
    column_count = HEADS * 2 * HEAD_DIM

    def project(items):
        block, index = items
        raw_keys = jnp.dot(block, key_weight, preferred_element_type=jnp.float32)
        raw_keys = raw_keys.reshape(block_rows, 2 * HEADS, HEAD_DIM)
        positions = index * block_rows + jnp.arange(block_rows, dtype=jnp.int32)
        key_rows = rotate(raw_keys, positions, HEAD_DIM)
        key_rows = key_rows.reshape(block_rows, column_count).astype(jnp.bfloat16)
        value_rows = jnp.dot(block, value_weight, preferred_element_type=jnp.float32).astype(jnp.bfloat16)
        return (key_rows, value_rows)
    key_list = []
    value_list = []
    read_list = []
    for seq_index in range(SEQS):
        blocks = layer_input[seq_index].reshape(N_SP, block_rows, D)
        key_blocks, value_blocks = lax.map(project, (blocks, jnp.arange(N_SP, dtype=jnp.int32)))
        key_rows = key_blocks.reshape(LEN, column_count)
        value_rows = value_blocks.reshape(LEN, column_count)
        query_row = new_queries[seq_index].astype(jnp.float32)

        def read_head(head):
            first = (head * 2 * HEAD_DIM).astype(jnp.int32)
            key_part = lax.dynamic_slice_in_dim(key_rows, first, 2 * HEAD_DIM, 1).astype(jnp.float32)
            key_part = key_part.reshape(LEN, 2, HEAD_DIM)
            value_part = lax.dynamic_slice_in_dim(value_rows, first, 2 * HEAD_DIM, 1).astype(jnp.float32)
            query_part = lax.dynamic_slice_in_dim(query_row, first, 2 * HEAD_DIM, 0).reshape(2, HEAD_DIM)
            scores = jnp.einsum('md,lmd->ml', query_part, key_part) * HEAD_DIM ** (-0.5)
            maps = jax.nn.softmax(scores, axis=-1)
            return jnp.einsum('ml,le->me', maps, value_part)
        read_list.append(lax.map(read_head, jnp.arange(HEADS, dtype=jnp.int32)))
        key_list.append(key_rows)
        value_list.append(value_rows)
    key_cache = jnp.stack(key_list, axis=0)
    value_cache = jnp.stack(value_list, axis=0)
    reads = jnp.stack(read_list, axis=0)
    diff = reads[:, :, 0] - lambdas[None, :, None] * reads[:, :, 1]
    normed = diff * lax.rsqrt(lax.optimization_barrier(jnp.mean(diff * diff, axis=-1, keepdims=True)) + 1e-06) * head_gain
    headed = normed.reshape(SEQS, column_count).astype(jnp.bfloat16)
    group_cols = column_count // N_TP
    grouped = headed.reshape(SEQS, N_TP, group_cols).astype(jnp.float32)
    weight_groups = out_weight.reshape(N_TP, group_cols, D).astype(jnp.float32)
    partials = jnp.einsum('stc,tcd->std', grouped, weight_groups).astype(jnp.bfloat16)
    mixed = lax.optimization_barrier(jnp.sum(partials.astype(jnp.float32), axis=1)).astype(jnp.bfloat16)
    return (key_cache, value_cache, mixed)
```

```python
import functools

import jax
import jax.numpy as jnp
import numpy as np
from jax import lax
from jax.experimental import pallas as pl
from jax.experimental.pallas import tpu as pltpu
from jax.sharding import PartitionSpec as P

MESH = pl.DeviceIdType.MESH
HEAD_DIM = 64
SUB = 48
NX = 4
VMEM = pl.BlockSpec(memory_space=pltpu.VMEM)
ANY = pl.BlockSpec(memory_space=pl.ANY)


def angle_tables(sp_count):
    lanes = np.arange(128)
    freqs = 10000.0 ** (-2.0 * (lanes % 32) / HEAD_DIM)
    sign = np.where(lanes % HEAD_DIM < HEAD_DIM // 2, -1.0, 1.0)

    def table(positions):
        angles = positions[:, None].astype(np.float64) * freqs[None, :]
        return [np.cos(angles).astype(np.float32), (sign * np.sin(angles)).astype(np.float32)]

    blocks = table(np.arange(sp_count) * (32 * SUB))
    subs = table(np.arange(32) * SUB)
    rows = table(np.arange(SUB))
    return blocks + subs + rows


def kernel(
    x_hbm, wk_hbm, wv_hbm, q_ref, bc, bs, sc, ss, rc, rs,
    k_hbm, v_hbm, part_ref,
    xbuf, wbuf, kst, vst,
    local_sem, lsend, lrecv, dsend, drecv, osem,
):
    sp = lax.axis_index("sp")
    tp = lax.axis_index("tp")
    x, c = tp // 2, lax.rem(tp, 2)
    right = lax.rem(x + 1, NX) * 2 + c
    left = lax.rem(x + NX - 1, NX) * 2 + c
    partner = x * 2 + (1 - c)

    barrier = pltpu.get_barrier_semaphore()
    for peer in (right, left, partner):
        pl.semaphore_signal(barrier, inc=1, device_id={"tp": peer}, device_id_type=MESH)

    mine = [
        pltpu.make_async_copy(x_hbm.at[pl.ds(96 * u, 96)], xbuf.at[u], local_sem.at[u])
        for u in range(2)
    ]
    weights = [
        pltpu.make_async_copy(w, wbuf.at[:, pl.ds(256 * n, 256)], local_sem.at[2 + n])
        for n, w in enumerate((wk_hbm, wv_hbm))
    ]
    for copy in mine + weights:
        copy.start()

    def remote(src, dst, send, recv, peer):
        return pltpu.make_async_remote_copy(
            src_ref=src, dst_ref=dst, send_sem=send, recv_sem=recv,
            device_id={"tp": peer}, device_id_type=MESH,
        )

    def link_copy(src_unit, src_half, q, way):
        return remote(
            xbuf.at[src_unit, pl.ds(SUB * src_half, SUB)],
            xbuf.at[4 + 2 * q, pl.ds(SUB * way, SUB)],
            lsend.at[q, way], lrecv.at[q, way], (right, left)[way],
        )

    def core_copy(unit, to_unit, n):
        return remote(xbuf.at[unit], xbuf.at[to_unit], dsend.at[n], drecv.at[n], partner)

    pl.semaphore_wait(barrier, 3)
    for copy in mine:
        copy.wait()
    for q in range(4):
        for way in range(2):
            s = (q + 2 * way) % 4
            link_copy(s // 2, s % 2, q, way).start()
    for n in range(2):
        core_copy(n, 2 + n, n).start()
    for copy in weights:
        copy.wait()

    lane = lax.broadcasted_iota(jnp.int32, (8, 256), 1)
    row = lax.broadcasted_iota(jnp.int32, (8, 256), 0)
    q_all = jnp.broadcast_to(q_ref[...].astype(jnp.float32), (8, 256))
    q8 = jnp.where(lane // HEAD_DIM == lax.rem(row, 4), q_all, 0.0).astype(jnp.bfloat16)
    base_c, base_s = bc[pl.ds(sp, 1), :], bs[pl.ds(sp, 1), :]
    low_half = lax.rem(lax.broadcasted_iota(jnp.int32, (96, 128), 1), HEAD_DIM) < HEAD_DIM // 2
    upper = lax.broadcasted_iota(jnp.int32, (8, 96), 0) < 4

    def out_copies(unit, places):
        return [
            pltpu.make_async_copy(
                st.at[unit, pl.ds(SUB * j, SUB)],
                hbm.at[pl.ds(places[j] * SUB, SUB)],
                osem.at[unit, 2 * j + n],
            )
            for j in range(2)
            for n, (st, hbm) in enumerate(((kst, k_hbm), (vst, v_hbm)))
        ]

    def compute(unit, places, carry):
        m, l, acc = carry
        raw = jnp.dot(xbuf[unit], wbuf[...], preferred_element_type=jnp.float32)
        cos, sin = [], []
        for place in places:
            c2, s2 = sc[pl.ds(place, 1), :], ss[pl.ds(place, 1), :]
            c12 = base_c * c2 - base_s * s2
            s12 = base_s * c2 + base_c * s2
            cos.append(c12 * rc[...] - s12 * rs[...])
            sin.append(s12 * rc[...] + c12 * rs[...])
        cos, sin = jnp.concatenate(cos, axis=0), jnp.concatenate(sin, axis=0)
        turned = []
        for h in range(2):
            k = raw[:, 128 * h : 128 * h + 128]
            other = jnp.where(low_half, pltpu.roll(k, 96, 1), pltpu.roll(k, 32, 1))
            turned.append((k * cos + other * sin).astype(jnp.bfloat16))
        keys = jnp.concatenate(turned, axis=1)
        values = raw[:, 256:].astype(jnp.bfloat16)
        kst[unit] = keys
        vst[unit] = values
        scores = lax.dot_general(
            q8, keys, (((1,), (1,)), ((), ())), preferred_element_type=jnp.float32
        ) * HEAD_DIM ** (-0.5)
        m_new = jnp.maximum(m, jnp.max(scores, axis=1, keepdims=True))
        p = jnp.exp(scores - m_new)
        alpha = jnp.exp(m - m_new)
        l = l * alpha + jnp.sum(p, axis=1, keepdims=True)
        p_high = p.astype(jnp.bfloat16).astype(jnp.float32)
        p8 = jnp.where(upper, p_high, p - p_high).astype(jnp.bfloat16)
        acc = acc * alpha + jnp.dot(p8, values, preferred_element_type=jnp.float32)
        return m_new, l, acc

    def places_near(u):
        core = lax.rem(c + u // 2, 2)
        first = (2 * x + core) * 4 + 2 * lax.rem(u, 2)
        return first, first + 1

    def places_far(q, core):
        chip_a = lax.rem(x + NX - 1 - q // 4, NX)
        chip_b = lax.rem(x + 1 + q // 4, NX)
        return (2 * chip_a + core) * 4 + lax.rem(q, 4), (2 * chip_b + core) * 4 + lax.rem(q + 2, 4)

    carry = (
        jnp.full((8, 1), -1e30, jnp.float32),
        jnp.zeros((8, 1), jnp.float32),
        jnp.zeros((8, 256), jnp.float32),
    )

    def near(u, carry):
        @pl.when(u >= 2)
        def _():
            core_copy(u - 2, u, u - 2).wait_recv()

        return compute(u, places_near(u), carry)

    carry = lax.fori_loop(0, 4, near, carry)

    def far(q, carry):
        for way in range(2):
            link_copy(0, 0, q, way).wait_recv()

        @pl.when(q < 2)
        def _():
            for way in range(2):
                link_copy(4 + 2 * q, way, q + 4, way).start()

        core_copy(4 + 2 * q, 5 + 2 * q, q + 2).start()

        def one(h, carry):
            @pl.when(h == 1)
            def _():
                core_copy(4 + 2 * q, 5 + 2 * q, q + 2).wait_recv()

            unit = 4 + 2 * q + h
            return compute(unit, places_far(q, lax.rem(c + h, 2)), carry)

        carry = lax.fori_loop(0, 2, one, carry)
        for u in (2 * q, 2 * q + 1):
            @pl.when(u < 4)
            def _(u=u):
                for copy in out_copies(u, places_near(u)):
                    copy.start()

        @pl.when(q >= 2)
        def _():
            for h in range(2):
                for copy in out_copies(2 * q + h, places_far(q - 2, lax.rem(c + h, 2))):
                    copy.start()

        return carry

    m, l, acc = lax.fori_loop(0, 6, far, carry)

    tot = acc[:4] + acc[4:]
    row4 = lax.broadcasted_iota(jnp.int32, (4, 128), 0)
    lane4 = lax.broadcasted_iota(jnp.int32, (4, 128), 1)
    part_ref[0:4] = jnp.where(row4 < 2, tot[:, :128], tot[:, 128:])
    part_ref[4:8] = jnp.where(lane4 < 64, m[:4], l[:4])

    def last_out(n, _):
        q, h = 4 + n // 2, lax.rem(n, 2)
        for copy in out_copies(4 + 2 * q + h, places_far(q, lax.rem(c + h, 2))):
            copy.start()
        return 0

    lax.fori_loop(0, 4, last_out, 0)

    def drain_links(q, _):
        for way in range(2):
            link_copy(0, 0, q, way).wait_send()
        return 0

    lax.fori_loop(0, 6, drain_links, 0)

    def drain_cores(n, _):
        core_copy(0, 0, n).wait_send()
        return 0

    lax.fori_loop(0, 8, drain_cores, 0)

    def drain_out(u, _):
        for copy in out_copies(u, (0, 0)):
            copy.wait()
        return 0

    lax.fori_loop(0, 16, drain_out, 0)


def gathered_read(rows, key_weight, value_weight, queries, tables):
    tables = [jnp.asarray(t) for t in tables]
    count = rows.shape[0] * 8
    return pl.pallas_call(
        kernel,
        out_shape=(
            jax.ShapeDtypeStruct((count, 256), jnp.bfloat16),
            jax.ShapeDtypeStruct((count, 256), jnp.bfloat16),
            jax.ShapeDtypeStruct((8, 128), jnp.float32),
        ),
        in_specs=[ANY, ANY, ANY, VMEM] + [VMEM] * 6,
        out_specs=(ANY, ANY, VMEM),
        scratch_shapes=[
            pltpu.VMEM((16, 96, rows.shape[1]), jnp.bfloat16),
            pltpu.VMEM((rows.shape[1], 512), jnp.bfloat16),
            pltpu.VMEM((16, 96, 256), jnp.bfloat16),
            pltpu.VMEM((16, 96, 256), jnp.bfloat16),
            pltpu.SemaphoreType.DMA((4,)),
            pltpu.SemaphoreType.DMA((6, 2)),
            pltpu.SemaphoreType.DMA((6, 2)),
            pltpu.SemaphoreType.DMA((8,)),
            pltpu.SemaphoreType.DMA((8,)),
            pltpu.SemaphoreType.DMA((16, 4)),
        ],
        compiler_params=pltpu.CompilerParams(collective_id=0, has_side_effects=True),
    )(rows, key_weight, value_weight, queries, *tables)


def copy_for_each(array, axis):
    copies = jnp.broadcast_to(array, (lax.axis_size(axis), *array.shape))
    return lax.all_to_all(copies, axis, split_axis=0, concat_axis=0, tiled=True)


def on_device(layer_input, key_weight, value_weight, new_queries, lambdas, head_gain, out_weight):
    tables = angle_tables(lax.axis_size("sp"))
    keys, values, part = gathered_read(
        layer_input[0], key_weight, value_weight, new_queries, tables
    )
    parts = copy_for_each(part, "sp")
    weighted, highest, totals = parts[:, :4], parts[:, 4:, :1], parts[:, 4:, 64:65]
    factor = jnp.exp(highest - jnp.max(highest, axis=0, keepdims=True))
    reads = jnp.sum(weighted * factor, axis=0) / jnp.sum(totals * factor, axis=0)
    reads = reads.reshape(2, 2, 128)
    diff = reads[:, 0] - lambdas[:, None] * reads[:, 1]
    normed = diff * lax.rsqrt(jnp.mean(diff * diff, axis=-1, keepdims=True) + 1e-06) * head_gain
    headed = normed.reshape(1, -1).astype(jnp.bfloat16)
    partials = jnp.dot(headed, out_weight, preferred_element_type=jnp.float32)
    partials = partials.astype(jnp.bfloat16)
    peers = lax.axis_size("tp")
    blocks = lax.all_to_all(partials.reshape(peers, 1, -1), "tp", 0, 0, tiled=True)
    mixed = jnp.sum(blocks.astype(jnp.float32), axis=0).astype(jnp.bfloat16)
    return keys[None], values[None], mixed


def solution(mesh):
    in_specs = (
        P("gr", ("sp", "tp"), None),
        P(None, "tp"),
        P(None, "tp"),
        P("gr", "tp"),
        P("tp"),
        P(),
        P("tp", None),
    )
    out_specs = (P("gr", "sp", "tp"), P("gr", "sp", "tp"), P("gr", "tp"))
    return jax.shard_map(
        on_device, mesh=mesh, in_specs=in_specs, out_specs=out_specs, check_vma=False
    )
```

```python
import functools

import jax
import jax.numpy as jnp
import numpy as np
from jax import lax
from jax.experimental import pallas as pl
from jax.experimental.pallas import tpu as pltpu
from jax.sharding import PartitionSpec as P

MESH = pl.DeviceIdType.MESH
HEAD_DIM = 64
SUB = 48
NX = 4
NY = 8
VMEM = pl.BlockSpec(memory_space=pltpu.VMEM)
ANY = pl.BlockSpec(memory_space=pl.ANY)


def angle_tables(sp_count):
    lanes = np.arange(128)
    freqs = 10000.0 ** (-2.0 * (lanes % 32) / HEAD_DIM)
    sign = np.where(lanes % HEAD_DIM < HEAD_DIM // 2, -1.0, 1.0)

    def table(positions):
        angles = positions[:, None].astype(np.float64) * freqs[None, :]
        return [np.cos(angles).astype(np.float32), (sign * np.sin(angles)).astype(np.float32)]

    blocks = table(np.arange(sp_count) * (32 * SUB))
    subs = table(np.arange(32) * SUB)
    rows = table(np.arange(SUB))
    return blocks + subs + rows


def kernel(
    x_hbm, wk_hbm, wv_hbm, q_ref, lam_ref, gain_ref, wo_hbm, bc, bs, sc, ss, rc, rs,
    k_hbm, v_hbm, mixed_ref,
    xbuf, wbuf, obuf, kst, vst, ybuf, zbuf, pbuf, sbuf,
    local_sem, lsend, lrecv, dsend, drecv, osem,
    ysend, yrecv, zsend, zrecv, psend, precv, token,
):
    sp = lax.axis_index("sp")
    tp = lax.axis_index("tp")
    x, c = tp // 2, lax.rem(tp, 2)
    right = lax.rem(x + 1, NX) * 2 + c
    left = lax.rem(x + NX - 1, NX) * 2 + c
    partner = x * 2 + (1 - c)
    z, y = sp // NY, lax.rem(sp, NY)
    depth = lax.axis_size("sp") // NY

    def near_y(step):
        return z * NY + lax.rem(y + step, NY)

    def tell(sem, step, along_y):
        if along_y:
            for way in (step, NY - step):
                pl.semaphore_signal(sem, inc=1, device_id={"sp": near_y(way)}, device_id_type=MESH)

        @pl.when(z >= step)
        def _():
            pl.semaphore_signal(sem, inc=1, device_id={"sp": sp - step * NY}, device_id_type=MESH)

        @pl.when(z + step < depth)
        def _():
            pl.semaphore_signal(sem, inc=1, device_id={"sp": sp + step * NY}, device_id_type=MESH)

    def told(step, along_y):
        below = jnp.where(z >= step, 1, 0)
        above = jnp.where(z + step < depth, 1, 0)
        return below + above + (2 if along_y else 0)

    barrier = pltpu.get_barrier_semaphore()
    for peer in (right, left, partner):
        pl.semaphore_signal(barrier, inc=1, device_id={"tp": peer}, device_id_type=MESH)
    tell(barrier, 1, True)

    mine = [
        pltpu.make_async_copy(x_hbm.at[pl.ds(96 * u, 96)], xbuf.at[u], local_sem.at[u])
        for u in range(2)
    ]
    weights = [
        pltpu.make_async_copy(w, wbuf.at[:, pl.ds(256 * n, 256)], local_sem.at[2 + n])
        for n, w in enumerate((wk_hbm, wv_hbm))
    ]
    projection = pltpu.make_async_copy(wo_hbm, obuf, local_sem.at[4])
    for copy in mine + weights + [projection]:
        copy.start()

    def remote(src, dst, send, recv, peer):
        return pltpu.make_async_remote_copy(
            src_ref=src, dst_ref=dst, send_sem=send, recv_sem=recv,
            device_id={"tp": peer}, device_id_type=MESH,
        )

    def link_copy(src_unit, src_half, q, way):
        return remote(
            xbuf.at[src_unit, pl.ds(SUB * src_half, SUB)],
            xbuf.at[4 + 2 * q, pl.ds(SUB * way, SUB)],
            lsend.at[q, way], lrecv.at[q, way], (right, left)[way],
        )

    def core_copy(unit, to_unit, n):
        return remote(xbuf.at[unit], xbuf.at[to_unit], dsend.at[n], drecv.at[n], partner)

    pl.semaphore_wait(barrier, 3 + told(1, True))
    for copy in mine:
        copy.wait()
    for q in range(4):
        for way in range(2):
            s = (q + 2 * way) % 4
            link_copy(s // 2, s % 2, q, way).start()
    for n in range(2):
        core_copy(n, 2 + n, n).start()
    tell(token.at[0], 1, True)
    for copy in weights:
        copy.wait()

    lane = lax.broadcasted_iota(jnp.int32, (8, 256), 1)
    row = lax.broadcasted_iota(jnp.int32, (8, 256), 0)
    q_all = jnp.broadcast_to(q_ref[...].astype(jnp.float32), (8, 256))
    q8 = jnp.where(lane // HEAD_DIM == lax.rem(row, 4), q_all, 0.0).astype(jnp.bfloat16)
    base_c, base_s = bc[pl.ds(sp, 1), :], bs[pl.ds(sp, 1), :]
    low_half = lax.rem(lax.broadcasted_iota(jnp.int32, (96, 128), 1), HEAD_DIM) < HEAD_DIM // 2
    upper = lax.broadcasted_iota(jnp.int32, (8, 96), 0) < 4

    def out_copies(unit, places):
        return [
            pltpu.make_async_copy(
                st.at[unit, pl.ds(SUB * j, SUB)],
                hbm.at[pl.ds(places[j] * SUB, SUB)],
                osem.at[unit, 2 * j + n],
            )
            for j in range(2)
            for n, (st, hbm) in enumerate(((kst, k_hbm), (vst, v_hbm)))
        ]

    def compute(unit, places, carry):
        m, l, acc = carry
        raw = jnp.dot(xbuf[unit], wbuf[...], preferred_element_type=jnp.float32)
        cos, sin = [], []
        for place in places:
            c2, s2 = sc[pl.ds(place, 1), :], ss[pl.ds(place, 1), :]
            c12 = base_c * c2 - base_s * s2
            s12 = base_s * c2 + base_c * s2
            cos.append(c12 * rc[...] - s12 * rs[...])
            sin.append(s12 * rc[...] + c12 * rs[...])
        cos, sin = jnp.concatenate(cos, axis=0), jnp.concatenate(sin, axis=0)
        turned = []
        for h in range(2):
            k = raw[:, 128 * h : 128 * h + 128]
            other = jnp.where(low_half, pltpu.roll(k, 96, 1), pltpu.roll(k, 32, 1))
            turned.append((k * cos + other * sin).astype(jnp.bfloat16))
        keys = jnp.concatenate(turned, axis=1)
        values = raw[:, 256:].astype(jnp.bfloat16)
        kst[unit] = keys
        vst[unit] = values
        scores = lax.dot_general(
            q8, keys, (((1,), (1,)), ((), ())), preferred_element_type=jnp.float32
        ) * HEAD_DIM ** (-0.5)
        m_new = jnp.maximum(m, jnp.max(scores, axis=1, keepdims=True))
        p = jnp.exp(scores - m_new)
        alpha = jnp.exp(m - m_new)
        l = l * alpha + jnp.sum(p, axis=1, keepdims=True)
        p_high = p.astype(jnp.bfloat16).astype(jnp.float32)
        p8 = jnp.where(upper, p_high, p - p_high).astype(jnp.bfloat16)
        acc = acc * alpha + jnp.dot(p8, values, preferred_element_type=jnp.float32)
        return m_new, l, acc

    def places_near(u):
        core = lax.rem(c + u // 2, 2)
        first = (2 * x + core) * 4 + 2 * lax.rem(u, 2)
        return first, first + 1

    def places_far(q, core):
        chip_a = lax.rem(x + NX - 1 - q // 4, NX)
        chip_b = lax.rem(x + 1 + q // 4, NX)
        return (2 * chip_a + core) * 4 + lax.rem(q, 4), (2 * chip_b + core) * 4 + lax.rem(q + 2, 4)

    carry = (
        jnp.full((8, 1), -1e30, jnp.float32),
        jnp.zeros((8, 1), jnp.float32),
        jnp.zeros((8, 256), jnp.float32),
    )

    def near(u, carry):
        @pl.when(u >= 2)
        def _():
            core_copy(u - 2, u, u - 2).wait_recv()

        return compute(u, places_near(u), carry)

    carry = lax.fori_loop(0, 4, near, carry)

    def far(q, carry):
        @pl.when(q == 1)
        def _():
            pl.semaphore_wait(token.at[0], told(1, True))
            tell(token.at[1], 2, True)

        @pl.when(q == 3)
        def _():
            pl.semaphore_wait(token.at[1], told(2, True))
            tell(token.at[2], 4, False)

        for way in range(2):
            link_copy(0, 0, q, way).wait_recv()

        @pl.when(q < 2)
        def _():
            for way in range(2):
                link_copy(4 + 2 * q, way, q + 4, way).start()

        core_copy(4 + 2 * q, 5 + 2 * q, q + 2).start()

        def one(h, carry):
            @pl.when(h == 1)
            def _():
                core_copy(4 + 2 * q, 5 + 2 * q, q + 2).wait_recv()

            unit = 4 + 2 * q + h
            return compute(unit, places_far(q, lax.rem(c + h, 2)), carry)

        carry = lax.fori_loop(0, 2, one, carry)
        for u in (2 * q, 2 * q + 1):
            @pl.when(u < 4)
            def _(u=u):
                for copy in out_copies(u, places_near(u)):
                    copy.start()

        @pl.when(q >= 2)
        def _():
            for h in range(2):
                for copy in out_copies(2 * q + h, places_far(q - 2, lax.rem(c + h, 2))):
                    copy.start()

        return carry

    m, l, acc = lax.fori_loop(0, 6, far, carry)

    tot = acc[:4] + acc[4:]
    row4 = lax.broadcasted_iota(jnp.int32, (4, 128), 0)
    lane4 = lax.broadcasted_iota(jnp.int32, (4, 128), 1)
    pl.semaphore_wait(token.at[2], told(4, False))

    def exchange(buf, mine_at, peers, send, recv, axis):
        return [
            pltpu.make_async_remote_copy(
                src_ref=buf.at[mine_at], dst_ref=buf.at[mine_at],
                send_sem=send.at[n], recv_sem=recv.at[mine_at],
                device_id={axis: peer}, device_id_type=MESH,
            )
            for n, peer in enumerate(peers)
        ]

    def arrived(buf, slots, send, recv, axis, peer):
        for slot in slots:
            pltpu.make_async_remote_copy(
                src_ref=buf.at[slot], dst_ref=buf.at[slot],
                send_sem=send.at[0], recv_sem=recv.at[slot],
                device_id={axis: peer}, device_id_type=MESH,
            ).wait_recv()

    def packed(weighted, highest, totals):
        ends = jnp.where(lane4 < 64, highest, totals)
        return jnp.concatenate([weighted, ends], axis=0)

    def combined(buf):
        parts = buf[...]
        highest, totals = parts[:, 4:, 0:1], parts[:, 4:, 64:65]
        top = jnp.max(highest, axis=0)
        factor = jnp.exp(highest - top[None])
        return jnp.sum(parts[:, :4] * factor, axis=0), top, jnp.sum(totals * factor, axis=0)

    ybuf[y] = packed(jnp.where(row4 < 2, tot[:, :128], tot[:, 128:]), m[:4], l[:4])
    y_slots = [lax.rem(y + k, NY) for k in range(1, NY)]
    y_peers = [near_y(k) for k in range(1, NY)]
    y_copies = exchange(ybuf, y, y_peers, ysend, yrecv, "sp")
    for copy in y_copies:
        copy.start()

    def last_out(n, _):
        q, h = 4 + n // 2, lax.rem(n, 2)
        for copy in out_copies(4 + 2 * q + h, places_far(q, lax.rem(c + h, 2))):
            copy.start()
        return 0

    lax.fori_loop(0, 4, last_out, 0)
    projection.wait()
    arrived(ybuf, y_slots, ysend, yrecv, "sp", y_peers[0])

    zbuf[z] = packed(*combined(ybuf))
    z_slots = [lax.rem(z + k, depth) for k in range(1, depth)]
    z_peers = [slot * NY + y for slot in z_slots]
    z_copies = exchange(zbuf, z, z_peers, zsend, zrecv, "sp")
    for copy in z_copies:
        copy.start()

    def drain_links(q, _):
        for way in range(2):
            link_copy(0, 0, q, way).wait_send()
        return 0

    lax.fori_loop(0, 6, drain_links, 0)

    def drain_cores(n, _):
        core_copy(0, 0, n).wait_send()
        return 0

    lax.fori_loop(0, 8, drain_cores, 0)

    def drain_out(u, _):
        for copy in out_copies(u, (0, 0)):
            copy.wait()
        return 0

    lax.fori_loop(0, 16, drain_out, 0)
    for copy in y_copies:
        copy.wait_send()
    arrived(zbuf, z_slots, zsend, zrecv, "sp", z_peers[0])

    weighted, _, totals = combined(zbuf)
    reads = weighted / totals
    headed = []
    for h in range(2):
        diff = reads[2 * h : 2 * h + 1] - lam_ref[h] * reads[2 * h + 1 : 2 * h + 2]
        mean = jnp.mean(diff * diff, axis=1, keepdims=True)
        headed.append(diff * lax.rsqrt(mean + 1e-06) * gain_ref[...])
    headed = jnp.broadcast_to(jnp.concatenate(headed, axis=1), (8, 256)).astype(jnp.bfloat16)
    partial = jnp.dot(headed, obuf[...], preferred_element_type=jnp.float32)
    partial = partial.astype(jnp.bfloat16).astype(jnp.float32)
    row8 = lax.broadcasted_iota(jnp.int32, (8, 128), 0)
    for peer in range(2 * NX):
        first = 256 * peer
        sbuf[peer] = jnp.where(
            row8 == 0, partial[:, first : first + 128], partial[:, first + 128 : first + 256]
        )
    p_copies, p_slots = [], []
    for n in range(1, 2 * NX):
        peer = lax.rem(tp + n, 2 * NX)
        p_slots.append(peer)
        p_copies.append(
            pltpu.make_async_remote_copy(
                src_ref=sbuf.at[peer], dst_ref=pbuf.at[tp],
                send_sem=psend.at[n - 1], recv_sem=precv.at[tp],
                device_id={"tp": peer}, device_id_type=MESH,
            )
        )
    for copy in p_copies:
        copy.start()
    pbuf[tp] = sbuf[tp]
    for copy in z_copies:
        copy.wait_send()
    arrived(pbuf, p_slots, psend, precv, "tp", p_slots[0])
    total = jnp.sum(pbuf[...], axis=0)
    mixed_ref[...] = jnp.concatenate([total[0:1], total[1:2]], axis=1).astype(jnp.bfloat16)
    for copy in p_copies:
        copy.wait_send()


def on_device(layer_input, key_weight, value_weight, new_queries, lambdas, head_gain, out_weight):
    sp_count = lax.axis_size("sp")
    rows = layer_input[0]
    tables = [jnp.asarray(t) for t in angle_tables(sp_count)]
    count = rows.shape[0] * 2 * NX
    dma = pltpu.SemaphoreType.DMA
    keys, values, mixed = pl.pallas_call(
        kernel,
        out_shape=(
            jax.ShapeDtypeStruct((count, 256), jnp.bfloat16),
            jax.ShapeDtypeStruct((count, 256), jnp.bfloat16),
            jax.ShapeDtypeStruct((1, 256), jnp.bfloat16),
        ),
        in_specs=[ANY, ANY, ANY, VMEM, pl.BlockSpec(memory_space=pltpu.SMEM), VMEM, ANY] + [VMEM] * 6,
        out_specs=(ANY, ANY, VMEM),
        scratch_shapes=[
            pltpu.VMEM((16, 96, rows.shape[1]), jnp.bfloat16),
            pltpu.VMEM((rows.shape[1], 512), jnp.bfloat16),
            pltpu.VMEM(out_weight.shape, jnp.bfloat16),
            pltpu.VMEM((16, 96, 256), jnp.bfloat16),
            pltpu.VMEM((16, 96, 256), jnp.bfloat16),
            pltpu.VMEM((NY, 8, 128), jnp.float32),
            pltpu.VMEM((sp_count // NY, 8, 128), jnp.float32),
            pltpu.VMEM((2 * NX, 8, 128), jnp.float32),
            pltpu.VMEM((2 * NX, 8, 128), jnp.float32),
            dma((5,)), dma((6, 2)), dma((6, 2)), dma((8,)), dma((8,)), dma((16, 4)),
            dma((NY,)), dma((NY,)), dma((sp_count // NY,)), dma((sp_count // NY,)),
            dma((2 * NX,)), dma((2 * NX,)),
            pltpu.SemaphoreType.REGULAR((3,)),
        ],
        compiler_params=pltpu.CompilerParams(collective_id=0, has_side_effects=True),
    )(
        rows, key_weight, value_weight, new_queries, lambdas, head_gain.reshape(1, -1), out_weight,
        *tables,
    )
    return keys[None], values[None], mixed


def solution(mesh):
    in_specs = (
        P("gr", ("sp", "tp"), None),
        P(None, "tp"),
        P(None, "tp"),
        P("gr", "tp"),
        P("tp"),
        P(),
        P("tp", None),
    )
    out_specs = (P("gr", "sp", "tp"), P("gr", "sp", "tp"), P("gr", "tp"))
    return jax.shard_map(
        on_device, mesh=mesh, in_specs=in_specs, out_specs=out_specs, check_vma=False
    )
```

```python
import jax
import jax.numpy as jnp
import numpy as np
from jax import lax
from jax.experimental import pallas as pl
from jax.experimental.pallas import tpu as pltpu
from jax.sharding import PartitionSpec as P

MESH = pl.DeviceIdType.MESH
HEAD_DIM = 64
GRAIN = 16
UNIT = 96
LATE = 2
PIECE = UNIT // LATE
NX = 4
NY = 8
VMEM = pl.BlockSpec(memory_space=pltpu.VMEM)
ANY = pl.BlockSpec(memory_space=pl.ANY)


def angle_table(sp_count):
    lanes = np.arange(128)
    freqs = 10000.0 ** (-2.0 * (lanes % 32) / HEAD_DIM)
    sign = np.where(lanes % HEAD_DIM < HEAD_DIM // 2, -1.0, 1.0)
    positions = np.concatenate(
        [np.arange(sp_count) * 16 * UNIT, np.arange(16 * UNIT // GRAIN) * GRAIN, np.arange(UNIT)]
    )
    angles = positions[:, None].astype(np.float64) * freqs[None, :]
    return np.concatenate([np.cos(angles), sign * np.sin(angles)], axis=1).astype(np.float32)


def kernel(
    x_hbm, wk_hbm, wv_hbm, q_hbm, lam_hbm, gain_hbm, wo_hbm, table_hbm,
    k_ref, v_ref, mixed_ref,
    xbuf, fbuf, wbuf, obuf, qbuf, gbuf, tbuf, ybuf, zbuf, pbuf, sbuf, lam_ref,
    local_sem, lsend, lrecv, fsend, frecv, dsend, drecv,
    ysend, yrecv, zsend, zrecv, psend, precv, token,
):
    sp = lax.axis_index("sp")
    tp = lax.axis_index("tp")
    x, c = tp // 2, lax.rem(tp, 2)
    right = lax.rem(x + 1, NX) * 2 + c
    left = lax.rem(x + NX - 1, NX) * 2 + c
    partner = x * 2 + (1 - c)
    z, y = sp // NY, lax.rem(sp, NY)
    depth = lax.axis_size("sp") // NY

    def near_y(step):
        return z * NY + lax.rem(y + step, NY)

    def tell(sem, step, along_y):
        if along_y:
            for way in (step, NY - step):
                pl.semaphore_signal(sem, inc=1, device_id={"sp": near_y(way)}, device_id_type=MESH)

        @pl.when(z >= step)
        def _():
            pl.semaphore_signal(sem, inc=1, device_id={"sp": sp - step * NY}, device_id_type=MESH)

        @pl.when(z + step < depth)
        def _():
            pl.semaphore_signal(sem, inc=1, device_id={"sp": sp + step * NY}, device_id_type=MESH)

    def told(step, along_y):
        below = jnp.where(z >= step, 1, 0)
        above = jnp.where(z + step < depth, 1, 0)
        return below + above + (2 if along_y else 0)

    barrier = pltpu.get_barrier_semaphore()
    for peer in (right, left, partner):
        pl.semaphore_signal(barrier, inc=1, device_id={"tp": peer}, device_id_type=MESH)
    tell(barrier, 1, True)

    mine = [
        pltpu.make_async_copy(x_hbm.at[pl.ds(UNIT * u, UNIT)], xbuf.at[u], local_sem.at[u])
        for u in range(2)
    ]
    rest = [
        pltpu.make_async_copy(src, dst, local_sem.at[2 + n])
        for n, (src, dst) in enumerate(
            (
                (wk_hbm, wbuf.at[:, pl.ds(0, 256)]),
                (wv_hbm, wbuf.at[:, pl.ds(256, 256)]),
                (q_hbm, qbuf),
                (table_hbm, tbuf),
                (lam_hbm, lam_ref),
                (gain_hbm, gbuf),
                (wo_hbm, obuf),
            )
        )
    ]
    for copy in mine + rest:
        copy.start()

    def remote(src, dst, send, recv, peer):
        return pltpu.make_async_remote_copy(
            src_ref=src, dst_ref=dst, send_sem=send, recv_sem=recv,
            device_id={"tp": peer}, device_id_type=MESH,
        )

    def link_copy(half, turn, way):
        return remote(
            xbuf.at[half], xbuf.at[4 + 4 * turn + 2 * way],
            lsend.at[turn, way], lrecv.at[turn, way], (right, left)[way],
        )

    def forward_copy(k, way):
        return remote(
            xbuf.at[4 + 2 * way, pl.ds(PIECE * k, PIECE)],
            fbuf.at[2 * k, pl.ds(PIECE * way, PIECE)],
            fsend.at[k, way], frecv.at[k, way], (right, left)[way],
        )

    def core_copy(unit, to_unit, n):
        return remote(xbuf.at[unit], xbuf.at[to_unit], dsend.at[n], drecv.at[n], partner)

    def late_core_copy(k):
        return remote(
            fbuf.at[2 * k], fbuf.at[2 * k + 1], dsend.at[6 + k], drecv.at[6 + k], partner
        )

    for copy in mine:
        copy.wait()
    pl.semaphore_wait(barrier, 3 + told(1, True))
    for turn in range(2):
        for way in range(2):
            link_copy((turn + way) % 2, turn, way).start()
    for n in range(2):
        core_copy(n, 2 + n, n).start()
    tell(token.at[0], 1, True)
    for copy in rest:
        copy.wait()

    lane = lax.broadcasted_iota(jnp.int32, (8, 256), 1)
    row = lax.broadcasted_iota(jnp.int32, (8, 256), 0)
    q_all = jnp.broadcast_to(qbuf[...].astype(jnp.float32), (8, 256))
    q8 = jnp.where(lane // HEAD_DIM == lax.rem(row, 4), q_all, 0.0).astype(jnp.bfloat16)
    sp_count = depth * NY
    base = tbuf[pl.ds(sp, 1), :]
    base_c, base_s = base[:, :128], base[:, 128:]
    sub_count = 16 * UNIT // GRAIN
    rows = tbuf[pl.ds(sp_count + sub_count, UNIT), :]

    def compute(unit_ref, places, carry):
        m, l, acc = carry
        size = unit_ref.shape[0]
        each = size // len(places)
        low_half = lax.rem(lax.broadcasted_iota(jnp.int32, (size, 128), 1), HEAD_DIM) < HEAD_DIM // 2
        upper = lax.broadcasted_iota(jnp.int32, (8, size), 0) < 4
        raw = jnp.dot(unit_ref[...], wbuf[...], preferred_element_type=jnp.float32)
        row_c, row_s = rows[:each, :128], rows[:each, 128:]
        cos, sin = [], []
        for place in places:
            sub = tbuf[pl.ds(sp_count + place, 1), :]
            c2, s2 = sub[:, :128], sub[:, 128:]
            c12 = base_c * c2 - base_s * s2
            s12 = base_s * c2 + base_c * s2
            cos.append(c12 * row_c - s12 * row_s)
            sin.append(s12 * row_c + c12 * row_s)
        cos, sin = jnp.concatenate(cos, axis=0), jnp.concatenate(sin, axis=0)
        turned = []
        for h in range(2):
            k = raw[:, 128 * h : 128 * h + 128]
            other = jnp.where(low_half, pltpu.roll(k, 96, 1), pltpu.roll(k, 32, 1))
            turned.append((k * cos + other * sin).astype(jnp.bfloat16))
        keys = jnp.concatenate(turned, axis=1)
        values = raw[:, 256:].astype(jnp.bfloat16)
        for j, place in enumerate(places):
            at = pl.ds(pl.multiple_of(place * GRAIN, GRAIN), each)
            k_ref[at] = keys[each * j : each * j + each]
            v_ref[at] = values[each * j : each * j + each]
        scores = lax.dot_general(
            q8, keys, (((1,), (1,)), ((), ())), preferred_element_type=jnp.float32
        ) * HEAD_DIM ** (-0.5)
        m_new = jnp.maximum(m, jnp.max(scores, axis=1, keepdims=True))
        p = jnp.exp(scores - m_new)
        alpha = jnp.exp(m - m_new)
        l = l * alpha + jnp.sum(p, axis=1, keepdims=True)
        p_high = p.astype(jnp.bfloat16).astype(jnp.float32)
        p8 = jnp.where(upper, p_high, p - p_high).astype(jnp.bfloat16)
        acc = acc * alpha + jnp.dot(p8, values, preferred_element_type=jnp.float32)
        return m_new, l, acc

    per_piece, per_half, per_late = 2 * UNIT // GRAIN, UNIT // GRAIN, PIECE // GRAIN

    def place_of(chip, core, half):
        return (2 * lax.rem(chip, NX) + core) * per_piece + half * per_half

    carry = (
        jnp.full((8, 1), -1e30, jnp.float32),
        jnp.zeros((8, 1), jnp.float32),
        jnp.zeros((8, 256), jnp.float32),
    )

    def near(u, carry):
        @pl.when(u >= 2)
        def _():
            core_copy(u - 2, u, u - 2).wait_recv()

        core = lax.rem(c + u // 2, 2)
        return compute(xbuf.at[u], [place_of(x, core, lax.rem(u, 2))], carry)

    carry = lax.fori_loop(0, 4, near, carry)
    pl.semaphore_wait(token.at[0], told(1, True))
    tell(token.at[1], 2, True)

    def far(turn, carry):
        @pl.when(turn == 1)
        def _():
            pl.semaphore_wait(token.at[1], told(2, True))
            tell(token.at[2], 4, False)

        for way in range(2):
            link_copy(0, turn, way).wait_recv()

            @pl.when(turn == 0)
            def _(way=way):
                for k in range(LATE):
                    forward_copy(k, way).start()

            core_copy(4 + 4 * turn + 2 * way, 5 + 4 * turn + 2 * way, 2 + 2 * turn + way).start()

        def one(n, carry):
            h, way = n // 2, lax.rem(n, 2)
            unit = 4 + 4 * turn + 2 * way + h

            @pl.when(h == 1)
            def _():
                core_copy(unit - 1, unit, 2 + 2 * turn + way).wait_recv()

            chip = jnp.where(way == 0, x + NX - 1, x + 1)
            place = place_of(chip, lax.rem(c + h, 2), lax.rem(turn + way, 2))
            return compute(xbuf.at[unit], [place], carry)

        return lax.fori_loop(0, 4, one, carry)

    carry = lax.fori_loop(0, 2, far, carry)

    def late(k, carry):
        for way in range(2):
            forward_copy(k, way).wait_recv()
        late_core_copy(k).start()

        def one(h, carry):
            @pl.when(h == 1)
            def _():
                late_core_copy(k).wait_recv()

            core = lax.rem(c + h, 2)
            places = [place_of(x + 2, core, way) + k * per_late for way in range(2)]
            return compute(fbuf.at[2 * k + h], places, carry)

        return lax.fori_loop(0, 2, one, carry)

    m, l, acc = lax.fori_loop(0, LATE, late, carry)

    tot = acc[:4] + acc[4:]
    row4 = lax.broadcasted_iota(jnp.int32, (4, 128), 0)
    lane4 = lax.broadcasted_iota(jnp.int32, (4, 128), 1)
    pl.semaphore_wait(token.at[2], told(4, False))

    def exchange(buf, mine_at, peers, send, recv, axis):
        return [
            pltpu.make_async_remote_copy(
                src_ref=buf.at[mine_at], dst_ref=buf.at[mine_at],
                send_sem=send.at[n], recv_sem=recv.at[mine_at],
                device_id={axis: peer}, device_id_type=MESH,
            )
            for n, peer in enumerate(peers)
        ]

    def arrived(buf, slots, send, recv, axis, peer):
        for slot in slots:
            pltpu.make_async_remote_copy(
                src_ref=buf.at[slot], dst_ref=buf.at[slot],
                send_sem=send.at[0], recv_sem=recv.at[slot],
                device_id={axis: peer}, device_id_type=MESH,
            ).wait_recv()

    def packed(weighted, highest, totals):
        ends = jnp.where(lane4 < 64, highest, totals)
        return jnp.concatenate([weighted, ends], axis=0)

    def combined(buf):
        parts = buf[...]
        highest, totals = parts[:, 4:, 0:1], parts[:, 4:, 64:65]
        top = jnp.max(highest, axis=0)
        factor = jnp.exp(highest - top[None])
        return jnp.sum(parts[:, :4] * factor, axis=0), top, jnp.sum(totals * factor, axis=0)

    ybuf[y] = packed(jnp.where(row4 < 2, tot[:, :128], tot[:, 128:]), m[:4], l[:4])
    y_order = sorted(range(1, NY), key=lambda k: -min(k, NY - k))
    y_slots = [lax.rem(y + k, NY) for k in y_order]
    y_peers = [near_y(k) for k in y_order]
    y_copies = exchange(ybuf, y, y_peers, ysend, yrecv, "sp")
    for copy in y_copies:
        copy.start()

    for way in range(2):
        for turn in range(2):
            link_copy(0, turn, way).wait_send()
        for k in range(LATE):
            forward_copy(k, way).wait_send()
    for n in range(6):
        core_copy(0, 0, n).wait_send()
    for k in range(LATE):
        late_core_copy(k).wait_send()
    arrived(ybuf, y_slots, ysend, yrecv, "sp", y_peers[0])

    zbuf[z] = packed(*combined(ybuf))
    above = depth - 1 - z
    z_slots = [jnp.where(n < above, depth - 1 - n, n - above) for n in range(depth - 1)]
    z_peers = [slot * NY + y for slot in z_slots]
    z_copies = exchange(zbuf, z, z_peers, zsend, zrecv, "sp")
    for copy in z_copies:
        copy.start()
    for copy in y_copies:
        copy.wait_send()
    arrived(zbuf, z_slots, zsend, zrecv, "sp", z_peers[0])

    weighted, _, totals = combined(zbuf)
    reads = weighted / totals
    headed = []
    for h in range(2):
        diff = reads[2 * h : 2 * h + 1] - lam_ref[h] * reads[2 * h + 1 : 2 * h + 2]
        mean = jnp.mean(diff * diff, axis=1, keepdims=True)
        headed.append(diff * lax.rsqrt(mean + 1e-06) * gbuf[...])
    headed = jnp.broadcast_to(jnp.concatenate(headed, axis=1), (8, 256)).astype(jnp.bfloat16)
    partial = jnp.dot(headed, obuf[...], preferred_element_type=jnp.float32)
    partial = partial.astype(jnp.bfloat16).astype(jnp.float32)
    row8 = lax.broadcasted_iota(jnp.int32, (8, 128), 0)
    for peer in range(2 * NX):
        first = 256 * peer
        sbuf[peer] = jnp.where(
            row8 == 0, partial[:, first : first + 128], partial[:, first + 128 : first + 256]
        )
    p_copies, p_slots = [], []
    for n, step in enumerate((4, 5, 3, 2, 6, 7, 1)):
        peer = lax.rem(tp + step, 2 * NX)
        p_slots.append(peer)
        p_copies.append(
            pltpu.make_async_remote_copy(
                src_ref=sbuf.at[peer], dst_ref=pbuf.at[tp],
                send_sem=psend.at[n], recv_sem=precv.at[tp],
                device_id={"tp": peer}, device_id_type=MESH,
            )
        )
    for copy in p_copies:
        copy.start()
    pbuf[tp] = sbuf[tp]
    for copy in z_copies + p_copies:
        copy.wait_send()
    arrived(pbuf, p_slots, psend, precv, "tp", p_slots[0])
    total = jnp.sum(pbuf[...], axis=0)
    mixed_ref[...] = jnp.concatenate([total[0:1], total[1:2]], axis=1).astype(jnp.bfloat16)


def write_out(k_ref, v_ref, mixed_ref, k_hbm, v_hbm, mixed_hbm, sem):
    copies = [
        pltpu.make_async_copy(src, dst, sem.at[n])
        for n, (src, dst) in enumerate(((k_ref, k_hbm), (v_ref, v_hbm), (mixed_ref, mixed_hbm)))
    ]
    for copy in copies:
        copy.start()
    for copy in copies:
        copy.wait()


def on_device(layer_input, key_weight, value_weight, new_queries, lambdas, head_gain, out_weight):
    sp_count = lax.axis_size("sp")
    rows = layer_input[0]
    table = jnp.asarray(angle_table(sp_count))
    shapes = [((rows.shape[0] * 2 * NX, 256), jnp.bfloat16)] * 2 + [((1, 256), jnp.bfloat16)]
    dma = pltpu.SemaphoreType.DMA
    in_vmem = pl.pallas_call(
        kernel,
        out_shape=tuple(pltpu.VMEM(*shape) for shape in shapes),
        in_specs=[ANY] * 8,
        out_specs=(VMEM,) * 3,
        scratch_shapes=[
            pltpu.VMEM((12, UNIT, rows.shape[1]), jnp.bfloat16),
            pltpu.VMEM((2 * LATE, 2 * PIECE, rows.shape[1]), jnp.bfloat16),
            pltpu.VMEM((rows.shape[1], 512), jnp.bfloat16),
            pltpu.VMEM(out_weight.shape, jnp.bfloat16),
            pltpu.VMEM((1, 256), jnp.bfloat16),
            pltpu.VMEM((1, 128), jnp.float32),
            pltpu.VMEM(table.shape, jnp.float32),
            pltpu.VMEM((NY, 8, 128), jnp.float32),
            pltpu.VMEM((sp_count // NY, 8, 128), jnp.float32),
            pltpu.VMEM((2 * NX, 8, 128), jnp.float32),
            pltpu.VMEM((2 * NX, 8, 128), jnp.float32),
            pltpu.SMEM((2,), jnp.float32),
            dma((9,)), dma((2, 2)), dma((2, 2)), dma((LATE, 2)), dma((LATE, 2)),
            dma((6 + LATE,)), dma((6 + LATE,)),
            dma((NY,)), dma((NY,)), dma((sp_count // NY,)), dma((sp_count // NY,)),
            dma((2 * NX,)), dma((2 * NX,)),
            pltpu.SemaphoreType.REGULAR((3,)),
        ],
        compiler_params=pltpu.CompilerParams(collective_id=0, has_side_effects=True),
    )(
        rows, key_weight, value_weight, new_queries, lambdas, head_gain.reshape(1, -1), out_weight,
        table,
    )
    keys, values, mixed = pl.pallas_call(
        write_out,
        out_shape=tuple(jax.ShapeDtypeStruct(*shape) for shape in shapes),
        in_specs=[VMEM] * 3,
        out_specs=(ANY,) * 3,
        scratch_shapes=[dma((3,))],
    )(*(pltpu.with_memory_space_constraint(a, pltpu.VMEM) for a in in_vmem))
    return keys[None], values[None], mixed


def solution(mesh):
    in_specs = (
        P("gr", ("sp", "tp"), None),
        P(None, "tp"),
        P(None, "tp"),
        P("gr", "tp"),
        P("tp"),
        P(),
        P("tp", None),
    )
    out_specs = (P("gr", "sp", "tp"), P("gr", "sp", "tp"), P("gr", "tp"))
    return jax.shard_map(
        on_device, mesh=mesh, in_specs=in_specs, out_specs=out_specs, check_vma=False
    )
```
